32 devices in a mesh: sp: 8 (over z, x), tp: 4 (over y, core).
Axes of the slice: x: 2, y: 2, z: 4, core: 2. Of those that a mesh axis runs over, the one named last changes fastest.
Arguments:
- query_small: bfloat16 [6144, 1024], P('sp', 'tp'), may hold values from -18 to 18
- key_small: bfloat16 [6144, 1024], P('sp', 'tp'), may hold values from -6 to 6
- value_small: bfloat16 [6144, 1024], P('sp', 'tp'), may hold values from -6 to 6
- offset_small: bfloat16 [16, 6144], P('tp', 'sp'), may hold values from -25 to 0
- query_large: bfloat16 [6144, 1024], P('sp', 'tp'), may hold values from -18 to 18
- key_large: bfloat16 [6144, 1024], P('sp', 'tp'), may hold values from -6 to 6
- value_large: bfloat16 [6144, 1024], P('sp', 'tp'), may hold values from -6 to 6
- offset_large: bfloat16 [8, 6144], P('tp', 'sp'), may hold values from -25 to 0
- out_small: bfloat16 [1024, 2048], P('tp'), may hold values from -0.125 to 0.125
- out_large: bfloat16 [1024, 2048], P('tp'), may hold values from -0.125 to 0.125
- residual: bfloat16 [6144, 2048], P(('sp', 'tp')), may hold values from -1.1953125 to 1.1953125
- norm_gain: bfloat16 [2048], replicated, may hold values from 0.099609375 to 1.8984375
- gate_weight: bfloat16 [2048, 5632], P('sp', 'tp'), may hold values from -0.125 to 0.125
- up_weight: bfloat16 [2048, 5632], P('sp', 'tp'), may hold values from -0.125 to 0.125
- down_weight: bfloat16 [5632, 2048], P('tp', 'sp'), may hold values from -0.078125 to 0.078125
Outputs:
- layer_out: bfloat16 [6144, 2048], P(('sp', 'tp'))
The draws below stay inside these ranges and needn't reach their ends.
All inputs are finite; a program needn't handle non-finite values.
Results may differ from the reference program's by a relative error of at most 0.023.
Values may be sent and summed in bfloat16 or wider, within the bound.
A program may use at most 128 MiB of HBM per device.

```python
import math
import jax
import jax.numpy as jnp
from jax import lax

D = 2048
HEADS_SMALL = 16
SMALL_DIM = 64
HEADS_LARGE = 8
LARGE_DIM = 128
FF = 5632
TOK_DEV = 768
SEQUENCE_LENGTH = 6144
N_TP = 4


def draw_offsets(key, head_count_list):
    random_keys = jax.random.split(key, 7)
    share = 0.5
    quick = jax.random.uniform(random_keys[0], (head_count_list,)) < share
    slow_base = math.log(0.35 / SEQUENCE_LENGTH) - 4.5 + jax.random.uniform(random_keys[1], (head_count_list,), minval=-0.5, maxval=0.5)
    quick_base = -8.4 + jax.random.uniform(random_keys[2], (head_count_list,), minval=-0.5, maxval=0.5)
    baseline_output = jnp.where(quick, quick_base, slow_base)
    position_shifts = jax.random.uniform(random_keys[3], (head_count_list, SEQUENCE_LENGTH // TOK_DEV), minval=-0.7, maxval=0.7)
    position_shifts = jnp.repeat(position_shifts, TOK_DEV, axis=1)
    approximate_output = jax.random.uniform(random_keys[4], (head_count_list, SEQUENCE_LENGTH), minval=-0.5, maxval=0.5)
    sample_spots = jax.random.randint(random_keys[5], (head_count_list, 3), 0, SEQUENCE_LENGTH)
    token_places = jnp.arange(SEQUENCE_LENGTH, dtype=jnp.int32)
    sample_draw = jnp.any(token_places[None, :, None] == sample_spots[:, None, :], axis=2)
    sample_draw_value = jax.random.uniform(random_keys[6], (head_count_list, SEQUENCE_LENGTH), minval=-1.5, maxval=-0.5)
    return jnp.where(sample_draw, sample_draw_value, baseline_output[:, None] + position_shifts + approximate_output).astype(jnp.float32)


def draw_offset_small(key, part):
    return draw_offsets(jax.random.fold_in(key, 11), HEADS_SMALL).astype(jnp.bfloat16)


def draw_offset_large(key, part):
    return draw_offsets(jax.random.fold_in(key, 23), HEADS_LARGE).astype(jnp.bfloat16)


def level_of(rng, extent, shards, least, largest):
    def one(dim, parts):
        steps = jax.random.uniform(jax.random.fold_in(jax.random.fold_in(rng, 6), dim), (parts,), jnp.float32, least / len(shards), largest / len(shards))
        return jnp.repeat(jnp.exp(steps), extent[dim] // parts).reshape((-1,) + (1,) * (len(extent) - dim - 1))

    factor_of = one(*shards[0])
    for cut in shards[1:]:
        factor_of = factor_of * one(*cut)
    return factor_of


def normal_values(rng, extent, width, limit, pieces=(), kind=jnp.bfloat16):
    result = width * jax.random.normal(rng, extent, jnp.float32)
    if pieces:
        result = result * level_of(rng, extent, pieces, -0.22, 0.18)
    return jnp.clip(result, -limit, limit).astype(kind)


def setup_inputs(seed: int = 0) -> dict:
    seeds = jax.random.split(jax.random.key(seed), 16)
    query_small = normal_values(seeds[0], (SEQUENCE_LENGTH, HEADS_SMALL * SMALL_DIM), 3.0, 18.0, ((0, 8), (1, 4)))
    key_small = normal_values(seeds[1], (SEQUENCE_LENGTH, HEADS_SMALL * SMALL_DIM), 1.0, 6.0, ((0, 8), (1, 4)))
    value_small = normal_values(seeds[2], (SEQUENCE_LENGTH, HEADS_SMALL * SMALL_DIM), 1.0, 6.0, ((0, 8), (1, 4)))
    offset_small = draw_offset_small(jax.random.fold_in(seeds[15], 71), 0)
    query_large = normal_values(seeds[4], (SEQUENCE_LENGTH, HEADS_LARGE * LARGE_DIM), 3.0, 18.0, ((0, 8), (1, 4)))
    key_large = normal_values(seeds[5], (SEQUENCE_LENGTH, HEADS_LARGE * LARGE_DIM), 1.0, 6.0, ((0, 8), (1, 4)))
    value_large = normal_values(seeds[6], (SEQUENCE_LENGTH, HEADS_LARGE * LARGE_DIM), 1.0, 6.0, ((0, 8), (1, 4)))
    offset_large = draw_offset_large(jax.random.fold_in(seeds[15], 71), 0)
    out_small = normal_values(seeds[8], (HEADS_SMALL * SMALL_DIM, D), (HEADS_SMALL * SMALL_DIM + HEADS_LARGE * LARGE_DIM) ** -0.5, 0.125, ((0, 4),))
    out_large = normal_values(seeds[9], (HEADS_LARGE * LARGE_DIM, D), (HEADS_SMALL * SMALL_DIM + HEADS_LARGE * LARGE_DIM) ** -0.5, 0.125, ((0, 4),))
    residual = normal_values(seeds[10], (SEQUENCE_LENGTH, D), 0.2, 1.1953125, ((0, 32),))
    norm_gain = jnp.clip(1.0 + 0.18 * jax.random.normal(seeds[11], (D,), jnp.float32), 0.099609375, 1.8984375).astype(jnp.bfloat16)
    gate_weight = normal_values(seeds[12], (D, FF), D ** -0.5, 0.125, ((0, 8), (1, 4)))
    up_weight = normal_values(seeds[13], (D, FF), D ** -0.5, 0.125, ((0, 8), (1, 4)))
    down_weight = normal_values(seeds[14], (FF, D), FF ** -0.5, 0.078125, ((0, 4), (1, 8)))
    return {"query_small": query_small, "key_small": key_small, "value_small": value_small, "offset_small": offset_small, "query_large": query_large, "key_large": key_large, "value_large": value_large, "offset_large": offset_large, "out_small": out_small, "out_large": out_large, "residual": residual, "norm_gain": norm_gain, "gate_weight": gate_weight, "up_weight": up_weight, "down_weight": down_weight}


def stick_group(query, random_keys, values, offset, head_depth):
    head_count_list = offset.shape[0]

    def per_head(args):
        head_query, head_keys, head_values, head_offset = args
        key_pos = jnp.arange(SEQUENCE_LENGTH, dtype=jnp.int32)

        def per_block(first_row):
            block_query = lax.dynamic_slice_in_dim(head_query, first_row, TOK_DEV, 0)
            logits = jnp.dot(block_query, head_keys.T, preferred_element_type=jnp.float32) * head_depth ** (-0.5)
            logits = logits + head_offset.astype(jnp.float32)[None, :]
            query_pos = first_row + jnp.arange(TOK_DEV, dtype=jnp.int32)
            before = key_pos[None, :] < query_pos[:, None]
            fail_all = jax.nn.log_sigmoid(-logits)
            log_pass = logits + fail_all
            log_fail = jnp.where(before, fail_all, 0.0)
            suffix = lax.cumsum(log_fail, axis=1, reverse=True) - log_fail
            weights = jnp.where(before, jnp.exp(log_pass + suffix), 0.0).astype(jnp.bfloat16)
            return jnp.dot(weights, head_values, preferred_element_type=jnp.float32).astype(jnp.bfloat16)
        starts = jnp.arange(SEQUENCE_LENGTH // TOK_DEV, dtype=jnp.int32) * TOK_DEV
        return lax.map(per_block, starts).reshape(SEQUENCE_LENGTH, head_depth)

    def split_heads(flat):
        return flat.reshape(SEQUENCE_LENGTH, head_count_list, head_depth).transpose(1, 0, 2)
    mixed = lax.map(per_head, (split_heads(query), split_heads(random_keys), split_heads(values), offset))
    return mixed.transpose(1, 0, 2).reshape(SEQUENCE_LENGTH, head_count_list * head_depth)

def rounded(value):
    return lax.optimization_barrier(value.astype(jnp.bfloat16)).astype(jnp.float32)

def reference(query_small, key_small, value_small, offset_small, query_large, key_large, value_large, offset_large, out_small, out_large, residual, norm_gain, gate_weight, up_weight, down_weight):
    mixed_small = stick_group(query_small, key_small, value_small, offset_small, SMALL_DIM)
    mixed_large = stick_group(query_large, key_large, value_large, offset_large, LARGE_DIM)
    small_run = HEADS_SMALL * SMALL_DIM // N_TP
    large_run = HEADS_LARGE * LARGE_DIM // N_TP
    total = jnp.zeros((SEQUENCE_LENGTH, D), jnp.float32)
    for group in range(N_TP):
        part = jnp.dot(mixed_small[:, group * small_run:(group + 1) * small_run], out_small[group * small_run:(group + 1) * small_run], preferred_element_type=jnp.float32)
        part = part + jnp.dot(mixed_large[:, group * large_run:(group + 1) * large_run], out_large[group * large_run:(group + 1) * large_run], preferred_element_type=jnp.float32)
        total = total + rounded(part)
    stream = residual.astype(jnp.float32) + rounded(total)
    scale = lax.rsqrt(lax.optimization_barrier(jnp.mean(stream * stream, axis=-1, keepdims=True)) + 1e-06)
    normed = (stream * scale * norm_gain.astype(jnp.float32)).astype(jnp.bfloat16)
    gate = jnp.dot(normed, gate_weight, preferred_element_type=jnp.float32)
    upper = jnp.dot(normed, up_weight, preferred_element_type=jnp.float32)
    hidden = (jax.nn.silu(gate) * upper).astype(jnp.bfloat16)
    hidden_run = FF // N_TP
    summed = jnp.zeros((SEQUENCE_LENGTH, D), jnp.float32)
    for group in range(N_TP):
        part = jnp.dot(hidden[:, group * hidden_run:(group + 1) * hidden_run], down_weight[group * hidden_run:(group + 1) * hidden_run], preferred_element_type=jnp.float32)
        summed = summed + rounded(part)
    return (stream + rounded(summed)).astype(jnp.bfloat16)
```

```python
import functools
import math

import jax
import jax.numpy as jnp
from jax import lax
from jax.experimental import pallas as pl
from jax.experimental.pallas import tpu as pltpu
from jax.sharding import PartitionSpec as P


SMALL_DIM = 64
LARGE_DIM = 128
TILE = 256
LANES = 128
LOG2E = math.log2(math.e)
OFFSET_ROWS = 16
MESH = pl.DeviceIdType.MESH


def dot_t(a, b):
    return lax.dot_general(a, b, (((1,), (1,)), ((), ())), preferred_element_type=jnp.float32)


def column_count(mesh):
    line = [getattr(d, "coords", None) for d in mesh.devices[:, 0].reshape(-1)]
    if line[0] is None or mesh.axis_names != ("sp", "tp"):
        return 1
    width = 1
    while width < len(line) and line[width][2] == line[0][2]:
        width += 1
    return width if len(line) % width == 0 else 1


def attend_kernel(
    n_sp,
    width,
    n_small,
    n_large,
    q_ref,
    own_ref,
    tri_ref,
    out_ref,
    qs_ref,
    acc_ref,
    carry_ref,
    kv_ref,
    local_sem,
    up_sem,
    row_sem,
    recv_sem,
):
    height = n_sp // width
    sp = lax.axis_index("sp")
    tp = lax.axis_index("tp")
    z, x = sp // width, sp % width
    tokens = q_ref.shape[0]
    tiles = tokens // TILE
    small_cols = n_small * SMALL_DIM
    n_pairs = small_cols // LANES
    large_cols = n_large * LARGE_DIM
    per_group = own_ref.shape[1] // TILE

    def send(source, block, target, send_sem):
        return pltpu.make_async_remote_copy(
            src_ref=source,
            dst_ref=kv_ref.at[block],
            send_sem=send_sem,
            recv_sem=recv_sem.at[block],
            device_id=(target, tp),
            device_id_type=MESH,
        )

    barrier = pltpu.get_barrier_semaphore()
    for other in range(n_sp):

        @pl.when(other != sp)
        def _(other=other):
            pl.semaphore_signal(barrier, inc=1, device_id=(other, tp), device_id_type=MESH)

    local = pltpu.make_async_copy(own_ref, kv_ref.at[sp], local_sem)
    local.start()
    pl.semaphore_wait(barrier, n_sp - 1)

    def sends(row, act, source=None):
        block = row * width + x
        origin = kv_ref.at[block] if source is None else source

        @pl.when(z < height - 1)
        def _():
            act(send(origin, block, sp + width, up_sem.at[row]))

        for column in range(width):

            @pl.when((column != x) & ((row < z) | (column > x)))
            def _(column=column):
                act(send(origin, block, z * width + column, row_sem.at[row, column]))

    sends(z, lambda copy: copy.start(), own_ref)

    lane = lax.broadcasted_iota(jnp.int32, (tokens, LANES), 1)
    low_rows = lane < SMALL_DIM
    low = low_rows[:TILE]
    zero = jnp.zeros((TILE, LANES), jnp.bfloat16)
    zero_rows = jnp.zeros((tokens, LANES), jnp.bfloat16)
    for pair in range(n_pairs):
        q = q_ref[:, pair * LANES : (pair + 1) * LANES]
        qs_ref[2 * pair] = jnp.where(low_rows, q, zero_rows)
        qs_ref[2 * pair + 1] = jnp.where(low_rows, zero_rows, q)
    for head in range(n_large):
        first = small_cols + head * LANES
        qs_ref[n_small + head] = q_ref[:, first : first + LANES]
    acc_ref[...] = jnp.zeros_like(acc_ref)
    carry_ref[...] = jnp.zeros_like(carry_ref)
    tri = tri_ref[...]

    def weights_of(head, q_rows, key, offset, scale, before):
        z = dot_t(qs_ref[head, q_rows, :], key) * scale + offset
        t = jnp.log(1.0 + jnp.exp2(-jnp.abs(z))) * LOG2E
        log_pass = jnp.minimum(z, 0.0) - t
        log_fail = log_pass - z
        if before is not None:
            log_fail = jnp.where(before, log_fail, 0.0)
        after = jnp.dot(log_fail.astype(jnp.bfloat16), tri, preferred_element_type=jnp.float32)
        carried = carry_ref[head, q_rows, :]
        weights = jnp.exp2(log_pass + after + carried)
        if before is not None:
            weights = jnp.where(before, weights, 0.0)
        carry_ref[head, q_rows, :] = carried + after[:, :1] + log_fail[:, :1]
        return weights.astype(jnp.bfloat16)

    def one_tile(block, q_tile, tile, before):
        q_rows = pl.ds(pl.multiple_of(q_tile * TILE, TILE), TILE)
        rows = pl.ds(pl.multiple_of(tile * TILE, TILE), TILE)
        group = pl.multiple_of(tokens + (tile // per_group) * OFFSET_ROWS, OFFSET_ROWS)
        lanes = pl.multiple_of((tile % per_group) * TILE, TILE)
        offsets = kv_ref[block, pl.ds(group, OFFSET_ROWS), pl.ds(lanes, TILE)]
        offsets = offsets.astype(jnp.float32) * LOG2E
        for pair in range(n_pairs):
            cols = slice(pair * LANES, (pair + 1) * LANES)
            v_cols = slice(small_cols + pair * LANES, small_cols + (pair + 1) * LANES)
            key = kv_ref[block, rows, cols]
            value = kv_ref[block, rows, v_cols]
            scale = LOG2E * SMALL_DIM**-0.5
            first = 2 * pair
            w0 = weights_of(first, q_rows, key, offsets[first : first + 1], scale, before)
            w1 = weights_of(first + 1, q_rows, key, offsets[first + 1 : first + 2], scale, before)
            acc_ref[q_rows, cols] += jnp.dot(
                w0, jnp.where(low, value, zero), preferred_element_type=jnp.float32
            ) + jnp.dot(w1, jnp.where(low, zero, value), preferred_element_type=jnp.float32)
        for head in range(n_large):
            k_cols = slice(2 * small_cols + head * LANES, 2 * small_cols + (head + 1) * LANES)
            v_first = 2 * small_cols + large_cols + head * LANES
            out_cols = slice(small_cols + head * LANES, small_cols + (head + 1) * LANES)
            place = n_small + head
            w = weights_of(
                place,
                q_rows,
                kv_ref[block, rows, k_cols],
                offsets[place : place + 1],
                LOG2E * LARGE_DIM**-0.5,
                before,
            )
            acc_ref[q_rows, out_cols] += jnp.dot(
                w, kv_ref[block, rows, v_first : v_first + LANES], preferred_element_type=jnp.float32
            )

    row_pos = lax.broadcasted_iota(jnp.int32, (TILE, TILE), 0)
    key_pos = lax.broadcasted_iota(jnp.int32, (TILE, TILE), 1)
    local.wait()

    def own_tile(q_tile, nothing):
        one_tile(sp, q_tile, q_tile, key_pos < row_pos)
        return nothing

    lax.fori_loop(0, tiles, own_tile, 0)

    def whole_block(block):
        def body(index, nothing):
            one_tile(block, index // tiles, tiles - 1 - index % tiles, None)
            return nothing

        lax.fori_loop(0, tiles * tiles, body, 0)

    def rest(q_tile, nothing):
        def inner(index, nothing):
            one_tile(sp, q_tile, q_tile - 1 - index, None)
            return nothing

        return lax.fori_loop(0, q_tile, inner, nothing)

    lax.fori_loop(1, tiles, rest, 0)

    def arrived(block):
        send(kv_ref.at[block], block, sp, up_sem.at[0]).wait_recv()

    def one_row(index, nothing):
        row = z - index

        @pl.when(index > 0)
        def _():
            arrived(row * width + x)
            sends(row, lambda copy: copy.start())

        def one_column(step, nothing):
            column = width - 1 - step
            block = row * width + column

            @pl.when((index > 0) | (column < x))
            def _():
                @pl.when(column != x)
                def _():
                    arrived(block)

                whole_block(block)

            return nothing

        return lax.fori_loop(0, width, one_column, nothing)

    lax.fori_loop(0, z + 1, one_row, 0)
    out_ref[...] = acc_ref[...].astype(jnp.bfloat16)

    def finish(row, nothing):
        sends(row, lambda copy: copy.wait_send())
        return nothing

    lax.fori_loop(0, z + 1, finish, 0)


def attend(n_sp, width, query, packed, n_small, n_large):
    tokens, cols = query.shape
    heads = n_small + n_large
    height = n_sp // width
    places = jnp.arange(TILE, dtype=jnp.int32)
    tri = (places[:, None] > places[None, :]).astype(jnp.bfloat16)
    vmem = pl.BlockSpec(memory_space=pltpu.VMEM)
    return pl.pallas_call(
        functools.partial(attend_kernel, n_sp, width, n_small, n_large),
        out_shape=jax.ShapeDtypeStruct((tokens, cols), jnp.bfloat16),
        in_specs=[vmem, pl.BlockSpec(memory_space=pl.ANY), vmem],
        out_specs=vmem,
        scratch_shapes=[
            pltpu.VMEM((heads, tokens, LANES), jnp.bfloat16),
            pltpu.VMEM((tokens, cols), jnp.float32),
            pltpu.VMEM((heads, tokens, 1), jnp.float32),
            pltpu.VMEM((n_sp,) + packed.shape, jnp.bfloat16),
            pltpu.SemaphoreType.DMA,
            pltpu.SemaphoreType.DMA((height,)),
            pltpu.SemaphoreType.DMA((height, width)),
            pltpu.SemaphoreType.DMA((n_sp,)),
        ],
        compiler_params=pltpu.CompilerParams(
            vmem_limit_bytes=48 * 1024 * 1024, collective_id=0, has_side_effects=True
        ),
        cost_estimate=pl.CostEstimate(
            flops=2 * 3 * heads * tokens * tokens * n_sp * TILE,
            bytes_accessed=8 * n_sp * tokens * cols,
            transcendentals=3 * heads * tokens * tokens * n_sp,
        ),
        name="stick_attend",
    )(query, packed, tri)


def pack(keys_values, offsets):
    rows = jnp.concatenate(keys_values, axis=1)
    tokens, cols = rows.shape
    heads = offsets.shape[0]
    groups = -(-tokens // (cols // TILE * TILE))
    span = cols // TILE * TILE
    flat = jnp.pad(offsets, ((0, OFFSET_ROWS - heads), (0, groups * span - tokens)))
    flat = flat.reshape(OFFSET_ROWS, groups, span).transpose(1, 0, 2)
    flat = flat.reshape(groups * OFFSET_ROWS, span)
    return jnp.concatenate([rows, jnp.pad(flat, ((0, 0), (0, cols - span)))], axis=0)


def rounded(value):
    return lax.optimization_barrier(value.astype(jnp.bfloat16)).astype(jnp.float32)


def rms_norm(stream, gain):
    scale = lax.rsqrt(jnp.mean(stream * stream, axis=-1, keepdims=True) + 1e-06)
    return (stream * scale * gain.astype(jnp.float32)).astype(jnp.bfloat16)


def on_device(n_sp, width, *args):
    return layer(n_sp, width, *args)


def layer(
    n_sp,
    width,
    query_small,
    key_small,
    value_small,
    offset_small,
    query_large,
    key_large,
    value_large,
    offset_large,
    out_small,
    out_large,
    residual,
    norm_gain,
    gate_weight,
    up_weight,
    down_weight,
):
    packed = pack(
        (key_small, value_small, key_large, value_large),
        jnp.concatenate([offset_small, offset_large], axis=0),
    )
    gate_full = lax.all_gather(gate_weight, "sp", axis=0, tiled=True)
    up_full = lax.all_gather(up_weight, "sp", axis=0, tiled=True)
    down_full = lax.all_gather(down_weight, "sp", axis=1, tiled=True)
    query = jnp.concatenate([query_small, query_large], axis=1)
    out_rows = jnp.concatenate([out_small, out_large], axis=0)
    mixed = attend(
        n_sp, width, query, packed, offset_small.shape[0], offset_large.shape[0]
    )
    attended = lax.psum_scatter(
        jnp.dot(mixed, out_rows, preferred_element_type=jnp.float32).astype(jnp.bfloat16),
        "tp",
        scatter_dimension=0,
        tiled=True,
    ).astype(jnp.float32)
    stream = residual.astype(jnp.float32) + rounded(attended)
    normed = rms_norm(stream, norm_gain)
    normed_rows = lax.all_gather(normed, "tp", axis=0, tiled=True)
    gate = jnp.dot(normed_rows, gate_full, preferred_element_type=jnp.float32)
    upper = jnp.dot(normed_rows, up_full, preferred_element_type=jnp.float32)
    hidden = (jax.nn.silu(gate) * upper).astype(jnp.bfloat16)
    summed = lax.psum_scatter(
        jnp.dot(hidden, down_full, preferred_element_type=jnp.float32).astype(jnp.bfloat16),
        "tp",
        scatter_dimension=0,
        tiled=True,
    ).astype(jnp.float32)
    return (stream + rounded(summed)).astype(jnp.bfloat16)


def solution(mesh):
    return jax.shard_map(
        functools.partial(on_device, mesh.shape["sp"], column_count(mesh)),
        mesh=mesh,
        in_specs=(
            P("sp", "tp"),
            P("sp", "tp"),
            P("sp", "tp"),
            P("tp", "sp"),
            P("sp", "tp"),
            P("sp", "tp"),
            P("sp", "tp"),
            P("tp", "sp"),
            P("tp", None),
            P("tp", None),
            P(("sp", "tp"), None),
            P(),
            P("sp", "tp"),
            P("sp", "tp"),
            P("tp", "sp"),
        ),
        out_specs=P(("sp", "tp"), None),
        check_vma=False,
    )
```

```python
import functools
import math

import jax
import jax.numpy as jnp
from jax import lax
from jax.experimental import pallas as pl
from jax.experimental.pallas import tpu as pltpu
from jax.sharding import PartitionSpec as P


SMALL_DIM = 64
LARGE_DIM = 128
TILE = 256
LANES = 128
LOG2E = math.log2(math.e)
OFFSET_ROWS = 16
MESH = pl.DeviceIdType.MESH


def dot_t(a, b):
    return lax.dot_general(a, b, (((1,), (1,)), ((), ())), preferred_element_type=jnp.float32)


def column_count(mesh):
    line = [getattr(d, "coords", None) for d in mesh.devices[:, 0].reshape(-1)]
    if line[0] is None or mesh.axis_names != ("sp", "tp"):
        return 1
    width = 1
    while width < len(line) and line[width][2] == line[0][2]:
        width += 1
    return width if len(line) % width == 0 else 1


def stick_attention(
    width,
    n_small,
    n_large,
    small_ref,
    large_ref,
    tri_ref,
    qs_ref,
    acc_ref,
    carry_ref,
    kv_ref,
    own_ready,
    arrived,
    forward,
    landed,
):
    sp = lax.axis_index("sp")
    z, x = sp // width, sp % width
    tokens = small_ref.shape[0]
    tiles = tokens // TILE
    small_cols = n_small * SMALL_DIM
    n_pairs = small_cols // LANES
    large_cols = n_large * LARGE_DIM
    per_group = kv_ref.shape[2] // TILE
    lane = lax.broadcasted_iota(jnp.int32, (tokens, LANES), 1)
    low_rows = lane < SMALL_DIM
    low = low_rows[:TILE]
    zero = jnp.zeros((TILE, LANES), jnp.bfloat16)
    zero_rows = jnp.zeros((tokens, LANES), jnp.bfloat16)
    for pair in range(n_pairs):
        q = small_ref[:, pair * LANES : (pair + 1) * LANES]
        qs_ref[2 * pair] = jnp.where(low_rows, q, zero_rows)
        qs_ref[2 * pair + 1] = jnp.where(low_rows, zero_rows, q)
    for head in range(n_large):
        qs_ref[n_small + head] = large_ref[:, head * LANES : (head + 1) * LANES]
    acc_ref[...] = jnp.zeros_like(acc_ref)
    carry_ref[...] = jnp.zeros_like(carry_ref)
    source = lax.broadcasted_iota(jnp.int32, (TILE, TILE), 0)
    target = lax.broadcasted_iota(jnp.int32, (TILE, TILE), 1)
    tri_ref[...] = (source > target).astype(jnp.bfloat16)

    def weights_of(head, q_rows, key, offset, scale, before):
        z = dot_t(qs_ref[head, q_rows, :], key) * scale + offset
        soft = jnp.maximum(jnp.log(1.0 + jnp.exp2(jnp.minimum(z, 126.0))) * LOG2E, z)
        log_pass = z - soft
        if before is not None:
            soft = jnp.where(before, soft, 0.0)
        after = jnp.dot(soft.astype(jnp.bfloat16), tri_ref[...], preferred_element_type=jnp.float32)
        carried = carry_ref[head, q_rows, :]
        weights = jnp.exp2(log_pass - (after + carried))
        if before is not None:
            weights = jnp.where(before, weights, 0.0)
        carry_ref[head, q_rows, :] = carried + after[:, :1] + soft[:, :1]
        return weights.astype(jnp.bfloat16)

    def one_tile(block, q_tile, tile, before, count=TILE):
        q_rows = pl.ds(pl.multiple_of(q_tile * TILE, TILE), count)
        rows = pl.ds(pl.multiple_of(tile * TILE, TILE), TILE)
        group = pl.multiple_of(tokens + (tile // per_group) * OFFSET_ROWS, OFFSET_ROWS)
        lanes = pl.multiple_of((tile % per_group) * TILE, TILE)
        offsets = kv_ref[block, pl.ds(group, OFFSET_ROWS), pl.ds(lanes, TILE)]
        offsets = offsets.astype(jnp.float32) * LOG2E
        for pair in range(n_pairs):
            cols = slice(pair * LANES, (pair + 1) * LANES)
            v_cols = slice(small_cols + pair * LANES, small_cols + (pair + 1) * LANES)
            key = kv_ref[block, rows, cols]
            value = kv_ref[block, rows, v_cols]
            scale = LOG2E * SMALL_DIM**-0.5
            first = 2 * pair
            w0 = weights_of(first, q_rows, key, offsets[first : first + 1], scale, before)
            w1 = weights_of(first + 1, q_rows, key, offsets[first + 1 : first + 2], scale, before)
            acc_ref[q_rows, cols] += jnp.dot(
                w0, jnp.where(low, value, zero), preferred_element_type=jnp.float32
            ) + jnp.dot(w1, jnp.where(low, zero, value), preferred_element_type=jnp.float32)
        for head in range(n_large):
            k_cols = slice(2 * small_cols + head * LANES, 2 * small_cols + (head + 1) * LANES)
            v_first = 2 * small_cols + large_cols + head * LANES
            out_cols = slice(small_cols + head * LANES, small_cols + (head + 1) * LANES)
            place = n_small + head
            w = weights_of(
                place,
                q_rows,
                kv_ref[block, rows, k_cols],
                offsets[place : place + 1],
                LOG2E * LARGE_DIM**-0.5,
                before,
            )
            acc_ref[q_rows, out_cols] += jnp.dot(
                w, kv_ref[block, rows, v_first : v_first + LANES], preferred_element_type=jnp.float32
            )

    row_pos = lax.broadcasted_iota(jnp.int32, (TILE, TILE), 0)
    key_pos = lax.broadcasted_iota(jnp.int32, (TILE, TILE), 1)
    own_ready()

    def own_tile(q_tile, nothing):
        one_tile(sp, q_tile, q_tile, key_pos < row_pos)
        return nothing

    lax.fori_loop(0, tiles, own_tile, 0)

    def whole_block(block):
        def body(index, nothing):
            one_tile(block, 0, tiles - 1 - index, None, tokens)
            return nothing

        lax.fori_loop(0, tiles, body, 0)

    def rest(q_tile, nothing):
        def inner(index, nothing):
            one_tile(sp, q_tile, q_tile - 1 - index, None)
            return nothing

        return lax.fori_loop(0, q_tile, inner, nothing)

    lax.fori_loop(1, tiles, rest, 0)

    def next_row(row):
        @pl.when(row > 0)
        def _():
            arrived((row - 1) * width + x)
            forward(row - 1)

    @pl.when(x == 0)
    def _():
        next_row(z)

    def one_row(index, nothing):
        row = z - index
        first_other = jnp.where(index == 0, x, jnp.where(x == width - 1, x, width)) - 1

        def one_column(step, nothing):
            column = width - 1 - step
            block = row * width + column

            @pl.when((index > 0) | (column < x))
            def _():
                @pl.when(column != x)
                def _():
                    arrived(block)
                    landed(block)

                @pl.when(column == first_other)
                def _():
                    next_row(row)

                whole_block(block)

            return nothing

        return lax.fori_loop(0, width, one_column, nothing)

    lax.fori_loop(0, z + 1, one_row, 0)


class Travel:
    def __init__(self, n_sp, width, own_ref, kv_ref, up_sem, row_sem, recv_sem, shifted):
        self.shifted = shifted
        self.n_sp, self.width = n_sp, width
        self.own_ref, self.kv_ref = own_ref, kv_ref
        self.up_sem, self.row_sem, self.recv_sem = up_sem, row_sem, recv_sem
        self.sp, self.tp = lax.axis_index("sp"), lax.axis_index("tp")
        self.z, self.x = self.sp // width, self.sp % width

    def send(self, source, block, target, send_sem):
        return pltpu.make_async_remote_copy(
            src_ref=source,
            dst_ref=self.kv_ref.at[block],
            send_sem=send_sem,
            recv_sem=self.recv_sem.at[block],
            device_id=(target, self.tp),
            device_id_type=MESH,
        )

    def sends(self, row, act, source=None):
        block = row * self.width + self.x
        origin = self.kv_ref.at[block] if source is None else source

        @pl.when(self.z < self.n_sp // self.width - 1)
        def _():
            act(self.send(origin, block, self.sp + self.width, self.up_sem.at[row]))

        for column in range(self.width):

            wanted = (column != self.x) & ((row < self.z) | (column > self.x))
            if self.shifted:
                wanted &= (row > 0) | (self.z == 0) | (self.x > 0)

            @pl.when(wanted)
            def _(column=column):
                target = self.z * self.width + column
                act(self.send(origin, block, target, self.row_sem.at[row, column]))

    def start_own(self):
        self.sends(self.z, lambda copy: copy.start(), self.own_ref)

    def forward(self, row):
        self.sends(row, lambda copy: copy.start())

    def arrived(self, block):
        self.send(self.kv_ref.at[block], block, self.sp, self.up_sem.at[0]).wait_recv()

    def finish(self):
        def one(row, nothing):
            self.sends(row, lambda copy: copy.wait_send())
            return nothing

        lax.fori_loop(0, self.z + 1, one, 0)


def attend_kernel(
    n_sp,
    width,
    n_small,
    n_large,
    small_ref,
    large_ref,
    own_ref,
    out_ref,
    tri_ref,
    qs_ref,
    acc_ref,
    carry_ref,
    kv_ref,
    local_sem,
    up_sem,
    row_sem,
    recv_sem,
):
    travel = Travel(n_sp, width, own_ref, kv_ref, up_sem, row_sem, recv_sem, False)
    barrier = pltpu.get_barrier_semaphore()
    for other in range(n_sp):

        @pl.when(other != travel.sp)
        def _(other=other):
            pl.semaphore_signal(
                barrier, inc=1, device_id=(other, travel.tp), device_id_type=MESH
            )

    local = pltpu.make_async_copy(own_ref, kv_ref.at[travel.sp], local_sem)
    local.start()
    pl.semaphore_wait(barrier, n_sp - 1)
    travel.start_own()
    stick_attention(
        width,
        n_small,
        n_large,
        small_ref,
        large_ref,
        tri_ref,
        qs_ref,
        acc_ref,
        carry_ref,
        kv_ref,
        local.wait,
        travel.arrived,
        travel.forward,
        lambda block: None,
    )
    out_ref[...] = acc_ref[...].astype(jnp.bfloat16)
    travel.finish()


def attend(n_sp, width, query_small, query_large, packed, n_small, n_large):
    tokens = query_small.shape[0]
    cols = query_small.shape[1] + query_large.shape[1]
    heads = n_small + n_large
    height = n_sp // width
    vmem = pl.BlockSpec(memory_space=pltpu.VMEM)
    return pl.pallas_call(
        functools.partial(attend_kernel, n_sp, width, n_small, n_large),
        out_shape=jax.ShapeDtypeStruct((tokens, cols), jnp.bfloat16),
        in_specs=[vmem, vmem, pl.BlockSpec(memory_space=pl.ANY)],
        out_specs=vmem,
        scratch_shapes=[
            pltpu.VMEM((TILE, TILE), jnp.bfloat16),
            pltpu.VMEM((heads, tokens, LANES), jnp.bfloat16),
            pltpu.VMEM((tokens, cols), jnp.float32),
            pltpu.VMEM((heads, tokens, 1), jnp.float32),
            pltpu.VMEM((n_sp,) + packed.shape, jnp.bfloat16),
            pltpu.SemaphoreType.DMA,
            pltpu.SemaphoreType.DMA((height,)),
            pltpu.SemaphoreType.DMA((height, width)),
            pltpu.SemaphoreType.DMA((n_sp,)),
        ],
        compiler_params=pltpu.CompilerParams(
            vmem_limit_bytes=48 * 1024 * 1024, collective_id=0, has_side_effects=True
        ),
        cost_estimate=pl.CostEstimate(
            flops=2 * 3 * heads * tokens * tokens * n_sp * TILE,
            bytes_accessed=8 * n_sp * tokens * cols,
            transcendentals=3 * heads * tokens * tokens * n_sp,
        ),
        name="stick_attend",
    )(query_small, query_large, packed)


def pack(keys_values, offsets):
    rows = jnp.concatenate(keys_values, axis=1)
    tokens, cols = rows.shape
    heads = offsets.shape[0]
    groups = -(-tokens // (cols // TILE * TILE))
    span = cols // TILE * TILE
    flat = jnp.pad(offsets, ((0, OFFSET_ROWS - heads), (0, groups * span - tokens)))
    flat = flat.reshape(OFFSET_ROWS, groups, span).transpose(1, 0, 2)
    flat = flat.reshape(groups * OFFSET_ROWS, span)
    return jnp.concatenate([rows, jnp.pad(flat, ((0, 0), (0, cols - span)))], axis=0)


def rounded(value):
    return lax.optimization_barrier(value.astype(jnp.bfloat16)).astype(jnp.float32)


def rms_norm(stream, gain):
    scale = lax.rsqrt(jnp.mean(stream * stream, axis=-1, keepdims=True) + 1e-06)
    return (stream * scale * gain.astype(jnp.float32)).astype(jnp.bfloat16)


def fits(n_sp, width, tokens, hidden):
    return (
        lax.axis_size("tp") == 4
        and width == 2
        and n_sp % 4 == 0
        and hidden % LANES == 0
        and tokens % (4 * OFFSET_ROWS) == 0
    )


def layer_kernel(
    n_sp,
    width,
    n_small,
    n_large,
    small_ref,
    large_ref,
    own_ref,
    out_small_ref,
    out_large_ref,
    residual_ref,
    gain_ref,
    gate_ref,
    up_ref,
    down_ref,
    out_ref,
    tri_ref,
    qs_ref,
    acc_ref,
    carry_ref,
    kv_ref,
    wg_ref,
    wu_ref,
    wd_ref,
    mixed_ref,
    core_out_ref,
    core_in_ref,
    side_out_ref,
    side_in_ref,
    normed_ref,
    stream_ref,
    swap_out_ref,
    swap_in_ref,
    sum_ref,
    sum_in_ref,
    local_sem,
    up_sem,
    row_sem,
    recv_sem,
    shift_sem,
    own_w_sem,
    column_w_sem,
    row_w_sem,
    recv_w_sem,
    core_sem,
    side_sem,
    gather_sem,
    pass_sem,
    gather_in_sem,
    swap_sem,
    sum_sem,
):
    travel = Travel(n_sp, width, own_ref, kv_ref, up_sem, row_sem, recv_sem, True)
    height = n_sp // width
    sp, tp, z, x = travel.sp, travel.tp, travel.z, travel.x
    y, core = tp // 2, tp % 2
    partner = y * 2 + 1 - core
    across = (1 - y) * 2 + core
    low = z % 2
    z_other = z - low + 1 - low
    depth = gate_ref.shape[0]
    share = wg_ref.shape[1]
    spare = gate_ref.shape[1] - share
    part = residual_ref.shape[0]

    barrier = pltpu.get_barrier_semaphore()
    for other in range(n_sp):

        @pl.when(other != sp)
        def _(other=other):
            pl.semaphore_signal(barrier, inc=1, device_id=(other, tp), device_id_type=MESH)

    for other in range(4):

        @pl.when(other != tp)
        def _(other=other):
            pl.semaphore_signal(barrier, inc=1, device_id=(sp, other), device_id_type=MESH)

    corner = z_other * width + x
    pl.semaphore_signal(barrier, inc=1, device_id=(corner, across), device_id_type=MESH)

    local = pltpu.make_async_copy(own_ref, kv_ref.at[sp], local_sem)
    local.start()

    def weight_ends(block, half):
        first = pl.multiple_of(half * spare, LANES)
        rows = pl.ds(pl.multiple_of(block * depth, depth), depth)
        return (
            (gate_ref.at[:, pl.ds(first, share)], wg_ref.at[rows, :]),
            (up_ref.at[:, pl.ds(first, share)], wu_ref.at[rows, :]),
            (down_ref.at[pl.ds(first, share), :], wd_ref.at[:, rows]),
        )

    own_weights = tuple(
        pltpu.make_async_copy(source, target, own_w_sem.at[i])
        for i, (source, target) in enumerate(weight_ends(sp, low))
    )
    for copy in own_weights:
        copy.start()
    pl.semaphore_wait(barrier, n_sp - 1 + 3 + 1)
    travel.start_own()

    def weight_copies(block, half, target, send_sems, held):
        return tuple(
            pltpu.make_async_remote_copy(
                src_ref=place if held else source,
                dst_ref=place,
                send_sem=send_sems.at[i],
                recv_sem=recv_w_sem.at[block, i],
                device_id=(target, tp),
                device_id_type=MESH,
            )
            for i, (source, place) in enumerate(weight_ends(block, half))
        )

    def column_weights(row, act):
        for copy in weight_copies(sp, row % 2, row * width + x, column_w_sem.at[row], False):
            act(copy)

    def row_weights(row, act, held):
        target = z * width + 1 - x
        for copy in weight_copies(row * width + x, low, target, row_w_sem.at[row], held):
            act(copy)

    def start(copy):
        copy.start()

    def wait_send(copy):
        copy.wait_send()

    def wait_recv(copy):
        copy.wait_recv()

    def weights_down(index, nothing):
        column_weights(z - 1 - index, start)
        return nothing

    lax.fori_loop(0, z, weights_down, 0)

    def pass_on(row):
        for copy in weight_copies(row * width + x, low, sp, column_w_sem.at[row], True):
            wait_recv(copy)
        row_weights(row, start, True)

    def from_above(index, nothing):
        pass_on(z + 1 + index)
        return nothing

    def last_sends():
        @pl.when(z < height - 1)
        def _():
            column_weights(z + 1, start)

        row_weights(z, start, False)
        lax.fori_loop(0, height - 1 - z, from_above, 0)

    def shift_copy():
        return travel.send(kv_ref.at[0], 0, sp + width, shift_sem)

    @pl.when(sp == 0)
    def _():
        last_sends()

    def forward(row):
        travel.forward(row)

        @pl.when((row == 0) & (x == 0))
        def _():
            last_sends()

    def landed(block):
        @pl.when((block == 0) & (x == 1))
        def _():
            @pl.when(z < height - 1)
            def _():
                shift_copy().start()

            last_sends()

    stick_attention(
        width,
        n_small,
        n_large,
        small_ref,
        large_ref,
        tri_ref,
        qs_ref,
        acc_ref,
        carry_ref,
        kv_ref,
        local.wait,
        travel.arrived,
        forward,
        landed,
    )
    mixed_ref[...] = acc_ref[...].astype(jnp.bfloat16)

    small_cols = out_small_ref.shape[0]

    def chunk_product(chunk):
        rows = pl.ds(pl.multiple_of(chunk * part, OFFSET_ROWS), part)
        return jnp.dot(
            mixed_ref[rows, :small_cols], out_small_ref[...], preferred_element_type=jnp.float32
        ) + jnp.dot(
            mixed_ref[rows, small_cols:], out_large_ref[...], preferred_element_type=jnp.float32
        )

    def to(place, block, source, target, send_sem, arrive_sem):
        return pltpu.make_async_remote_copy(
            src_ref=source,
            dst_ref=target,
            send_sem=send_sem,
            recv_sem=arrive_sem,
            device_id=(place, block),
            device_id_type=MESH,
        )

    core_copies = tuple(
        to(sp, partner, core_out_ref.at[i], core_in_ref.at[i], core_sem.at[0, i], core_sem.at[1, i])
        for i in range(2)
    )
    side_copy = to(sp, across, side_out_ref, side_in_ref, side_sem.at[0], side_sem.at[1])
    core_out_ref[0] = chunk_product((1 - y) * 2 + 1 - core).astype(jnp.bfloat16)
    core_copies[0].start()
    stream_ref[...] = chunk_product(across)
    core_copies[0].wait_recv()
    side_out_ref[...] = (stream_ref[...] + core_in_ref[0].astype(jnp.float32)).astype(jnp.bfloat16)
    side_copy.start()
    core_out_ref[1] = chunk_product(y * 2 + 1 - core).astype(jnp.bfloat16)
    core_copies[1].start()
    stream_ref[...] = chunk_product(tp)
    core_copies[1].wait_recv()
    stream_ref[...] += core_in_ref[1].astype(jnp.float32)
    side_copy.wait_recv()
    attended = (stream_ref[...] + side_in_ref[...].astype(jnp.float32)).astype(jnp.bfloat16)
    stream = residual_ref[...].astype(jnp.float32) + attended.astype(jnp.float32)
    stream_ref[...] = stream
    scale = lax.rsqrt(jnp.mean(stream * stream, axis=-1, keepdims=True) + 1e-06)
    my_rows = pl.ds(pl.multiple_of(core * part, OFFSET_ROWS), part)
    other_rows = pl.ds(pl.multiple_of((1 - core) * part, OFFSET_ROWS), part)
    my_chip = low * 2 + y
    normed_ref[my_chip, my_rows, :] = (
        stream_ref[...] * scale * gain_ref[...].astype(jnp.float32)
    ).astype(jnp.bfloat16)

    def chip_of(step):
        dz, dy = 1 - step // 2, 1 - step % 2
        low_there = (low + dz) % 2
        y_there = (y + dy) % 2
        place = (z - low + low_there) * width + x
        return low_there * 2 + y_there, place, y_there * 2 + core

    def spread(step):
        _, place, block = chip_of(step)
        here = normed_ref.at[my_chip, my_rows, :]
        return to(place, block, here, here, gather_sem.at[step], gather_in_sem.at[my_chip, 0])

    def to_partner(chip, step):
        here = normed_ref.at[chip, my_rows, :]
        return to(sp, partner, here, here, pass_sem.at[step], gather_in_sem.at[chip, 1])

    def from_partner(chip):
        here = normed_ref.at[chip, other_rows, :]
        return to(sp, partner, here, here, pass_sem.at[0], gather_in_sem.at[chip, 1])

    for step in (2, 1, 0):
        spread(step).start()
    to_partner(my_chip, 3).start()

    def far_up(index, nothing):
        column_weights(height - 1 - index, start)
        return nothing

    def from_below(index, nothing):
        pass_on(z - 1 - index)
        return nothing

    lax.fori_loop(0, height - 2 - z, far_up, 0)
    lax.fori_loop(0, z, from_below, 0)
    for step in (2, 1, 0):
        chip, _, _ = chip_of(step)
        here = normed_ref.at[chip, my_rows, :]
        to(sp, partner, here, here, gather_sem.at[step], gather_in_sem.at[chip, 0]).wait_recv()
        to_partner(chip, step).start()

    for copy in own_weights:
        copy.wait()

    def row_arrived(row, nothing):
        for copy in weight_copies(row * width + 1 - x, low, sp, row_w_sem.at[row], True):
            wait_recv(copy)
        return nothing

    lax.fori_loop(0, height, row_arrived, 0)
    place_of = lax.broadcasted_iota(jnp.int32, (2 * part, share), 1)
    counted = place_of >= low * (share - spare)

    def swap_copy(step):
        return to(
            sp, partner, swap_out_ref.at[step], swap_in_ref.at[step], swap_sem.at[0, step], swap_sem.at[1, step]
        )

    def sum_copy(step):
        _, place, block = chip_of(step)
        return to(place, block, sum_ref.at[step], sum_in_ref.at[step], sum_sem.at[0, step], sum_sem.at[1, step])

    def add_partner(step):
        swap_copy(step).wait_recv()
        total = sum_ref[step].astype(jnp.float32) + swap_in_ref[step].astype(jnp.float32)
        sum_ref[step] = total.astype(jnp.bfloat16)

    def feed(step, nothing):
        chip, _, _ = chip_of(step)
        from_partner(chip).wait_recv()
        rows = normed_ref[chip]
        gate = jnp.dot(rows, wg_ref[...], preferred_element_type=jnp.float32)
        upper = jnp.dot(rows, wu_ref[...], preferred_element_type=jnp.float32)
        hidden = jnp.where(counted, jax.nn.silu(gate) * upper, 0.0).astype(jnp.bfloat16)
        down = jnp.dot(hidden, wd_ref[...], preferred_element_type=jnp.float32)
        first = down[:part].astype(jnp.bfloat16)
        second = down[part:].astype(jnp.bfloat16)

        @pl.when(core == 0)
        def _():
            sum_ref[step] = first
            swap_out_ref[step] = second

        @pl.when(core == 1)
        def _():
            sum_ref[step] = second
            swap_out_ref[step] = first

        swap_copy(step).start()

        @pl.when(step > 0)
        def _():
            add_partner(step - 1)
            sum_copy(step - 1).start()

        return nothing

    lax.fori_loop(0, 4, feed, 0)
    add_partner(3)
    total = sum_ref[3].astype(jnp.float32)
    for step in range(3):
        sum_copy(step).wait_recv()
        total += sum_in_ref[step].astype(jnp.float32)
    mixer = total.astype(jnp.bfloat16).astype(jnp.float32)
    out_ref[...] = (stream_ref[...] + mixer).astype(jnp.bfloat16)

    travel.finish()

    @pl.when((x == 1) & (z < height - 1))
    def _():
        shift_copy().wait_send()

    for copy in core_copies:
        wait_send(copy)
    wait_send(side_copy)
    for step in range(3):
        wait_send(spread(step))
        wait_send(sum_copy(step))
    for step in range(4):
        wait_send(to_partner(my_chip, step))
        wait_send(swap_copy(step))

    def weights_sent(row, nothing):
        @pl.when(row != z)
        def _():
            column_weights(row, wait_send)

        row_weights(row, wait_send, True)
        return nothing

    lax.fori_loop(0, height, weights_sent, 0)


def fused_layer(
    n_sp,
    width,
    query_small,
    query_large,
    packed,
    n_small,
    n_large,
    out_small,
    out_large,
    residual,
    norm_gain,
    gate_weight,
    up_weight,
    down_weight,
):
    tokens = query_small.shape[0]
    cols = query_small.shape[1] + query_large.shape[1]
    heads = n_small + n_large
    height = n_sp // width
    part, model = residual.shape
    hidden = gate_weight.shape[1]
    share = -(-hidden // (2 * LANES)) * LANES
    vmem = pl.BlockSpec(memory_space=pltpu.VMEM)
    hbm = pl.BlockSpec(memory_space=pl.ANY)
    piece = (part, model)
    bf16 = jnp.bfloat16
    dma = pltpu.SemaphoreType.DMA
    return pl.pallas_call(
        functools.partial(layer_kernel, n_sp, width, n_small, n_large),
        out_shape=jax.ShapeDtypeStruct(piece, bf16),
        in_specs=[vmem, vmem, hbm, vmem, vmem, vmem, vmem, hbm, hbm, hbm],
        out_specs=vmem,
        scratch_shapes=[
            pltpu.VMEM((TILE, TILE), bf16),
            pltpu.VMEM((heads, tokens, LANES), bf16),
            pltpu.VMEM((tokens, cols), jnp.float32),
            pltpu.VMEM((heads, tokens, 1), jnp.float32),
            pltpu.VMEM((n_sp,) + packed.shape, bf16),
            pltpu.VMEM((model, share), bf16),
            pltpu.VMEM((model, share), bf16),
            pltpu.VMEM((share, model), bf16),
            pltpu.VMEM((tokens, cols), bf16),
            pltpu.VMEM((2,) + piece, bf16),
            pltpu.VMEM((2,) + piece, bf16),
            pltpu.VMEM(piece, bf16),
            pltpu.VMEM(piece, bf16),
            pltpu.VMEM((4, 2 * part, model), bf16),
            pltpu.VMEM(piece, jnp.float32),
            pltpu.VMEM((4,) + piece, bf16),
            pltpu.VMEM((4,) + piece, bf16),
            pltpu.VMEM((4,) + piece, bf16),
            pltpu.VMEM((3,) + piece, bf16),
            dma,
            dma((height,)),
            dma((height, width)),
            dma((n_sp,)),
            dma,
            dma((3,)),
            dma((height, 3)),
            dma((height, 3)),
            dma((n_sp, 3)),
            dma((2, 2)),
            dma((2,)),
            dma((3,)),
            dma((4,)),
            dma((4, 2)),
            dma((2, 4)),
            dma((2, 3)),
        ],
        compiler_params=pltpu.CompilerParams(
            vmem_limit_bytes=67043328, collective_id=1, has_side_effects=True
        ),
        name="fused_layer",
    )(
        query_small,
        query_large,
        packed,
        out_small,
        out_large,
        residual,
        norm_gain.reshape(1, model),
        gate_weight,
        up_weight,
        down_weight,
    )


def on_device(n_sp, width, *args):
    return layer(n_sp, width, *args)


def layer(
    n_sp,
    width,
    query_small,
    key_small,
    value_small,
    offset_small,
    query_large,
    key_large,
    value_large,
    offset_large,
    out_small,
    out_large,
    residual,
    norm_gain,
    gate_weight,
    up_weight,
    down_weight,
):
    if fits(n_sp, width, value_small.shape[0], gate_weight.shape[1]):
        return fused_layer(
            n_sp,
            width,
            query_small,
            query_large,
            pack(
                (key_small, value_small, key_large, value_large),
                jnp.concatenate([offset_small, offset_large], axis=0),
            ),
            offset_small.shape[0],
            offset_large.shape[0],
            out_small,
            out_large,
            residual,
            norm_gain,
            gate_weight,
            up_weight,
            down_weight,
        )
    packed = pack(
        (key_small, value_small, key_large, value_large),
        jnp.concatenate([offset_small, offset_large], axis=0),
    )
    gate_full = lax.all_gather(gate_weight, "sp", axis=0, tiled=True)
    up_full = lax.all_gather(up_weight, "sp", axis=0, tiled=True)
    down_full = lax.all_gather(down_weight, "sp", axis=1, tiled=True)
    out_rows = jnp.concatenate([out_small, out_large], axis=0)
    mixed = attend(
        n_sp, width, query_small, query_large, packed, offset_small.shape[0], offset_large.shape[0]
    )
    attended = lax.psum_scatter(
        jnp.dot(mixed, out_rows, preferred_element_type=jnp.float32).astype(jnp.bfloat16),
        "tp",
        scatter_dimension=0,
        tiled=True,
    ).astype(jnp.float32)
    stream = residual.astype(jnp.float32) + rounded(attended)
    normed = rms_norm(stream, norm_gain)
    normed_rows = lax.all_gather(normed, "tp", axis=0, tiled=True)
    gate = jnp.dot(normed_rows, gate_full, preferred_element_type=jnp.float32)
    upper = jnp.dot(normed_rows, up_full, preferred_element_type=jnp.float32)
    hidden = (jax.nn.silu(gate) * upper).astype(jnp.bfloat16)
    summed = lax.psum_scatter(
        jnp.dot(hidden, down_full, preferred_element_type=jnp.float32).astype(jnp.bfloat16),
        "tp",
        scatter_dimension=0,
        tiled=True,
    ).astype(jnp.float32)
    return (stream + rounded(summed)).astype(jnp.bfloat16)


def solution(mesh):
    return jax.shard_map(
        functools.partial(on_device, mesh.shape["sp"], column_count(mesh)),
        mesh=mesh,
        in_specs=(
            P("sp", "tp"),
            P("sp", "tp"),
            P("sp", "tp"),
            P("tp", "sp"),
            P("sp", "tp"),
            P("sp", "tp"),
            P("sp", "tp"),
            P("tp", "sp"),
            P("tp", None),
            P("tp", None),
            P(("sp", "tp"), None),
            P(),
            P("sp", "tp"),
            P("sp", "tp"),
            P("tp", "sp"),
        ),
        out_specs=P(("sp", "tp"), None),
        check_vma=False,
    )
```

```python
import functools
import math

import jax
import jax.numpy as jnp
from jax import lax
from jax.experimental import pallas as pl
from jax.experimental.pallas import tpu as pltpu
from jax.sharding import PartitionSpec as P


SMALL_DIM = 64
LARGE_DIM = 128
TILE = 256
LANES = 128
LOG2E = math.log2(math.e)
OFFSET_ROWS = 16
MESH = pl.DeviceIdType.MESH


def dot_t(a, b):
    return lax.dot_general(a, b, (((1,), (1,)), ((), ())), preferred_element_type=jnp.float32)


def column_count(mesh):
    line = [getattr(d, "coords", None) for d in mesh.devices[:, 0].reshape(-1)]
    if line[0] is None or mesh.axis_names != ("sp", "tp"):
        return 1
    width = 1
    while width < len(line) and line[width][2] == line[0][2]:
        width += 1
    return width if len(line) % width == 0 else 1


def stick_attention(
    width,
    n_small,
    n_large,
    small_ref,
    large_ref,
    tri_ref,
    qs_ref,
    acc_ref,
    carry_ref,
    kv_ref,
    own_ready,
    arrived,
    forward,
    landed,
):
    sp = lax.axis_index("sp")
    z, x = sp // width, sp % width
    tokens = small_ref.shape[0]
    tiles = tokens // TILE
    small_cols = n_small * SMALL_DIM
    n_pairs = small_cols // LANES
    large_cols = n_large * LARGE_DIM
    per_group = kv_ref.shape[2] // TILE
    lane = lax.broadcasted_iota(jnp.int32, (tokens, LANES), 1)
    low_rows = lane < SMALL_DIM
    low = low_rows[:TILE]
    zero = jnp.zeros((TILE, LANES), jnp.bfloat16)
    zero_rows = jnp.zeros((tokens, LANES), jnp.bfloat16)
    for pair in range(n_pairs):
        q = small_ref[:, pair * LANES : (pair + 1) * LANES]
        qs_ref[2 * pair] = jnp.where(low_rows, q, zero_rows)
        qs_ref[2 * pair + 1] = jnp.where(low_rows, zero_rows, q)
    for head in range(n_large):
        qs_ref[n_small + head] = large_ref[:, head * LANES : (head + 1) * LANES]
    acc_ref[...] = jnp.zeros_like(acc_ref)
    carry_ref[...] = jnp.zeros_like(carry_ref)
    source = lax.broadcasted_iota(jnp.int32, (TILE, TILE), 0)
    target = lax.broadcasted_iota(jnp.int32, (TILE, TILE), 1)
    tri_ref[...] = (source > target).astype(jnp.bfloat16)

    def weights_of(head, q_rows, key, offset, scale, before):
        z = dot_t(qs_ref[head, q_rows, :], key) * scale + offset
        soft = jnp.maximum(jnp.log(1.0 + jnp.exp2(jnp.minimum(z, 126.0))) * LOG2E, z)
        log_pass = z - soft
        if before is not None:
            soft = jnp.where(before, soft, 0.0)
        after = jnp.dot(soft.astype(jnp.bfloat16), tri_ref[...], preferred_element_type=jnp.float32)
        carried = carry_ref[head, q_rows, :]
        weights = jnp.exp2(log_pass - (after + carried))
        if before is not None:
            weights = jnp.where(before, weights, 0.0)
        carry_ref[head, q_rows, :] = carried + after[:, :1] + soft[:, :1]
        return weights.astype(jnp.bfloat16)

    def one_tile(block, q_tile, tile, before, count=TILE):
        q_rows = pl.ds(pl.multiple_of(q_tile * TILE, TILE), count)
        rows = pl.ds(pl.multiple_of(tile * TILE, TILE), TILE)
        group = pl.multiple_of(tokens + (tile // per_group) * OFFSET_ROWS, OFFSET_ROWS)
        lanes = pl.multiple_of((tile % per_group) * TILE, TILE)
        offsets = kv_ref[block, pl.ds(group, OFFSET_ROWS), pl.ds(lanes, TILE)]
        offsets = offsets.astype(jnp.float32) * LOG2E
        for pair in range(n_pairs):
            cols = slice(pair * LANES, (pair + 1) * LANES)
            v_cols = slice(small_cols + pair * LANES, small_cols + (pair + 1) * LANES)
            key = kv_ref[block, rows, cols]
            value = kv_ref[block, rows, v_cols]
            scale = LOG2E * SMALL_DIM**-0.5
            first = 2 * pair
            w0 = weights_of(first, q_rows, key, offsets[first : first + 1], scale, before)
            w1 = weights_of(first + 1, q_rows, key, offsets[first + 1 : first + 2], scale, before)
            acc_ref[q_rows, cols] += jnp.dot(
                w0, jnp.where(low, value, zero), preferred_element_type=jnp.float32
            ) + jnp.dot(w1, jnp.where(low, zero, value), preferred_element_type=jnp.float32)
        for head in range(n_large):
            k_cols = slice(2 * small_cols + head * LANES, 2 * small_cols + (head + 1) * LANES)
            v_first = 2 * small_cols + large_cols + head * LANES
            out_cols = slice(small_cols + head * LANES, small_cols + (head + 1) * LANES)
            place = n_small + head
            w = weights_of(
                place,
                q_rows,
                kv_ref[block, rows, k_cols],
                offsets[place : place + 1],
                LOG2E * LARGE_DIM**-0.5,
                before,
            )
            acc_ref[q_rows, out_cols] += jnp.dot(
                w, kv_ref[block, rows, v_first : v_first + LANES], preferred_element_type=jnp.float32
            )

    row_pos = lax.broadcasted_iota(jnp.int32, (TILE, TILE), 0)
    key_pos = lax.broadcasted_iota(jnp.int32, (TILE, TILE), 1)
    own_ready()

    def own_tile(q_tile, nothing):
        one_tile(sp, q_tile, q_tile, key_pos < row_pos)
        return nothing

    lax.fori_loop(0, tiles, own_tile, 0)

    def whole_block(block):
        def body(index, nothing):
            one_tile(block, 0, tiles - 1 - index, None, tokens)
            return nothing

        lax.fori_loop(0, tiles, body, 0)

    def rest(q_tile, nothing):
        def inner(index, nothing):
            one_tile(sp, q_tile, q_tile - 1 - index, None)
            return nothing

        return lax.fori_loop(0, q_tile, inner, nothing)

    lax.fori_loop(1, tiles, rest, 0)

    def next_row(row):
        @pl.when(row > 0)
        def _():
            arrived((row - 1) * width + x)
            forward(row - 1)

    @pl.when(x == 0)
    def _():
        next_row(z)

    def one_row(index, nothing):
        row = z - index
        first_other = jnp.where(index == 0, x, jnp.where(x == width - 1, x, width)) - 1

        def one_column(step, nothing):
            column = width - 1 - step
            block = row * width + column

            @pl.when((index > 0) | (column < x))
            def _():
                @pl.when(column != x)
                def _():
                    arrived(block)
                    landed(block)

                @pl.when(column == first_other)
                def _():
                    next_row(row)

                whole_block(block)

            return nothing

        return lax.fori_loop(0, width, one_column, nothing)

    lax.fori_loop(0, z + 1, one_row, 0)


class Travel:
    def __init__(self, n_sp, width, own_ref, kv_ref, up_sem, row_sem, recv_sem, shifted):
        self.shifted = shifted
        self.n_sp, self.width = n_sp, width
        self.own_ref, self.kv_ref = own_ref, kv_ref
        self.up_sem, self.row_sem, self.recv_sem = up_sem, row_sem, recv_sem
        self.sp, self.tp = lax.axis_index("sp"), lax.axis_index("tp")
        self.z, self.x = self.sp // width, self.sp % width

    def send(self, source, block, target, send_sem):
        return pltpu.make_async_remote_copy(
            src_ref=source,
            dst_ref=self.kv_ref.at[block],
            send_sem=send_sem,
            recv_sem=self.recv_sem.at[block],
            device_id=(target, self.tp),
            device_id_type=MESH,
        )

    def sends(self, row, act, source=None):
        block = row * self.width + self.x
        origin = self.kv_ref.at[block] if source is None else source

        @pl.when(self.z < self.n_sp // self.width - 1)
        def _():
            act(self.send(origin, block, self.sp + self.width, self.up_sem.at[row]))

        for column in range(self.width):

            wanted = (column != self.x) & ((row < self.z) | (column > self.x))
            if self.shifted:
                last = self.z == self.n_sp // self.width - 1
                wanted &= (row > 0) | ~last | (self.x > 0)

            @pl.when(wanted)
            def _(column=column):
                target = self.z * self.width + column
                act(self.send(origin, block, target, self.row_sem.at[row, column]))

    def start_own(self):
        self.sends(self.z, lambda copy: copy.start(), self.own_ref)

    def forward(self, row):
        self.sends(row, lambda copy: copy.start())

    def arrived(self, block):
        self.send(self.kv_ref.at[block], block, self.sp, self.up_sem.at[0]).wait_recv()

    def finish(self):
        def one(row, nothing):
            self.sends(row, lambda copy: copy.wait_send())
            return nothing

        lax.fori_loop(0, self.z + 1, one, 0)


def attend_kernel(
    n_sp,
    width,
    n_small,
    n_large,
    small_ref,
    large_ref,
    own_ref,
    out_ref,
    tri_ref,
    qs_ref,
    acc_ref,
    carry_ref,
    kv_ref,
    local_sem,
    up_sem,
    row_sem,
    recv_sem,
):
    travel = Travel(n_sp, width, own_ref, kv_ref, up_sem, row_sem, recv_sem, False)
    barrier = pltpu.get_barrier_semaphore()
    for other in range(n_sp):

        @pl.when(other != travel.sp)
        def _(other=other):
            pl.semaphore_signal(
                barrier, inc=1, device_id=(other, travel.tp), device_id_type=MESH
            )

    local = pltpu.make_async_copy(own_ref, kv_ref.at[travel.sp], local_sem)
    local.start()
    pl.semaphore_wait(barrier, n_sp - 1)
    travel.start_own()
    stick_attention(
        width,
        n_small,
        n_large,
        small_ref,
        large_ref,
        tri_ref,
        qs_ref,
        acc_ref,
        carry_ref,
        kv_ref,
        local.wait,
        travel.arrived,
        travel.forward,
        lambda block: None,
    )
    out_ref[...] = acc_ref[...].astype(jnp.bfloat16)
    travel.finish()


def attend(n_sp, width, query_small, query_large, packed, n_small, n_large):
    tokens = query_small.shape[0]
    cols = query_small.shape[1] + query_large.shape[1]
    heads = n_small + n_large
    height = n_sp // width
    vmem = pl.BlockSpec(memory_space=pltpu.VMEM)
    return pl.pallas_call(
        functools.partial(attend_kernel, n_sp, width, n_small, n_large),
        out_shape=jax.ShapeDtypeStruct((tokens, cols), jnp.bfloat16),
        in_specs=[vmem, vmem, pl.BlockSpec(memory_space=pl.ANY)],
        out_specs=vmem,
        scratch_shapes=[
            pltpu.VMEM((TILE, TILE), jnp.bfloat16),
            pltpu.VMEM((heads, tokens, LANES), jnp.bfloat16),
            pltpu.VMEM((tokens, cols), jnp.float32),
            pltpu.VMEM((heads, tokens, 1), jnp.float32),
            pltpu.VMEM((n_sp,) + packed.shape, jnp.bfloat16),
            pltpu.SemaphoreType.DMA,
            pltpu.SemaphoreType.DMA((height,)),
            pltpu.SemaphoreType.DMA((height, width)),
            pltpu.SemaphoreType.DMA((n_sp,)),
        ],
        compiler_params=pltpu.CompilerParams(
            vmem_limit_bytes=48 * 1024 * 1024, collective_id=0, has_side_effects=True
        ),
        cost_estimate=pl.CostEstimate(
            flops=2 * 3 * heads * tokens * tokens * n_sp * TILE,
            bytes_accessed=8 * n_sp * tokens * cols,
            transcendentals=3 * heads * tokens * tokens * n_sp,
        ),
        name="stick_attend",
    )(query_small, query_large, packed)


def pack(keys_values, offsets):
    rows = jnp.concatenate(keys_values, axis=1)
    tokens, cols = rows.shape
    heads = offsets.shape[0]
    groups = -(-tokens // (cols // TILE * TILE))
    span = cols // TILE * TILE
    flat = jnp.pad(offsets, ((0, OFFSET_ROWS - heads), (0, groups * span - tokens)))
    flat = flat.reshape(OFFSET_ROWS, groups, span).transpose(1, 0, 2)
    flat = flat.reshape(groups * OFFSET_ROWS, span)
    return jnp.concatenate([rows, jnp.pad(flat, ((0, 0), (0, cols - span)))], axis=0)


def rounded(value):
    return lax.optimization_barrier(value.astype(jnp.bfloat16)).astype(jnp.float32)


def rms_norm(stream, gain):
    scale = lax.rsqrt(jnp.mean(stream * stream, axis=-1, keepdims=True) + 1e-06)
    return (stream * scale * gain.astype(jnp.float32)).astype(jnp.bfloat16)


def fits(n_sp, width, tokens, hidden):
    return (
        lax.axis_size("tp") == 4
        and width == 2
        and n_sp % 4 == 0
        and hidden % LANES == 0
        and tokens % (4 * OFFSET_ROWS) == 0
    )


def layer_kernel(
    n_sp,
    width,
    n_small,
    n_large,
    small_ref,
    large_ref,
    own_ref,
    out_small_ref,
    out_large_ref,
    residual_ref,
    gain_ref,
    gate_ref,
    up_ref,
    down_ref,
    out_ref,
    tri_ref,
    qs_ref,
    acc_ref,
    carry_ref,
    kv_ref,
    wg_ref,
    wu_ref,
    wd_ref,
    mixed_ref,
    core_out_ref,
    core_in_ref,
    side_out_ref,
    side_in_ref,
    normed_ref,
    stream_ref,
    swap_out_ref,
    swap_in_ref,
    sum_ref,
    sum_in_ref,
    local_sem,
    up_sem,
    row_sem,
    recv_sem,
    shift_sem,
    own_w_sem,
    column_w_sem,
    row_w_sem,
    recv_w_sem,
    core_sem,
    side_sem,
    gather_sem,
    pass_sem,
    gather_in_sem,
    swap_sem,
    sum_sem,
):
    travel = Travel(n_sp, width, own_ref, kv_ref, up_sem, row_sem, recv_sem, True)
    height = n_sp // width
    sp, tp, z, x = travel.sp, travel.tp, travel.z, travel.x
    y, core = tp // 2, tp % 2
    partner = y * 2 + 1 - core
    across = (1 - y) * 2 + core
    low = z % 2
    z_other = z - low + 1 - low
    depth = gate_ref.shape[0]
    share = wg_ref.shape[1]
    spare = gate_ref.shape[1] - share
    part = residual_ref.shape[0]

    barrier = pltpu.get_barrier_semaphore()
    for other in range(n_sp):

        @pl.when(other != sp)
        def _(other=other):
            pl.semaphore_signal(barrier, inc=1, device_id=(other, tp), device_id_type=MESH)

    for other in range(4):

        @pl.when(other != tp)
        def _(other=other):
            pl.semaphore_signal(barrier, inc=1, device_id=(sp, other), device_id_type=MESH)

    corner = z_other * width + x
    pl.semaphore_signal(barrier, inc=1, device_id=(corner, across), device_id_type=MESH)

    local = pltpu.make_async_copy(own_ref, kv_ref.at[sp], local_sem)
    local.start()

    def weight_ends(block, half):
        first = pl.multiple_of(half * spare, LANES)
        rows = pl.ds(pl.multiple_of(block * depth, depth), depth)
        return (
            (gate_ref.at[:, pl.ds(first, share)], wg_ref.at[rows, :]),
            (up_ref.at[:, pl.ds(first, share)], wu_ref.at[rows, :]),
            (down_ref.at[pl.ds(first, share), :], wd_ref.at[:, rows]),
        )

    own_weights = tuple(
        pltpu.make_async_copy(source, target, own_w_sem.at[i])
        for i, (source, target) in enumerate(weight_ends(sp, low))
    )
    for copy in own_weights:
        copy.start()
    pl.semaphore_wait(barrier, n_sp - 1 + 3 + 1)
    travel.start_own()

    def weight_copies(block, half, target, send_sems, held):
        return tuple(
            pltpu.make_async_remote_copy(
                src_ref=place if held else source,
                dst_ref=place,
                send_sem=send_sems.at[i],
                recv_sem=recv_w_sem.at[block, i],
                device_id=(target, tp),
                device_id_type=MESH,
            )
            for i, (source, place) in enumerate(weight_ends(block, half))
        )

    def column_weights(row, act):
        for copy in weight_copies(sp, row % 2, row * width + x, column_w_sem.at[row], False):
            act(copy)

    def row_weights(row, act, held):
        target = z * width + 1 - x
        for copy in weight_copies(row * width + x, low, target, row_w_sem.at[row], held):
            act(copy)

    def start(copy):
        copy.start()

    def wait_send(copy):
        copy.wait_send()

    def wait_recv(copy):
        copy.wait_recv()

    def weights_down(index, nothing):
        column_weights(z - 1 - index, start)
        return nothing

    lax.fori_loop(0, z, weights_down, 0)

    def pass_on(row):
        for copy in weight_copies(row * width + x, low, sp, column_w_sem.at[row], True):
            wait_recv(copy)
        row_weights(row, start, True)

    def from_above(index, nothing):
        pass_on(z + 1 + index)
        return nothing

    def last_sends():
        @pl.when(z < height - 1)
        def _():
            column_weights(z + 1, start)

        row_weights(z, start, False)
        lax.fori_loop(0, height - 1 - z, from_above, 0)

    def shift_copy():
        return travel.send(kv_ref.at[0], 0, sp + width, shift_sem)

    @pl.when(sp == 0)
    def _():
        last_sends()

    def forward(row):
        travel.forward(row)

        @pl.when((row == 0) & (x == 0))
        def _():
            last_sends()

    def landed(block):
        @pl.when((block == 0) & (x == 1))
        def _():
            @pl.when(z == height - 2)
            def _():
                shift_copy().start()

            last_sends()

    stick_attention(
        width,
        n_small,
        n_large,
        small_ref,
        large_ref,
        tri_ref,
        qs_ref,
        acc_ref,
        carry_ref,
        kv_ref,
        local.wait,
        travel.arrived,
        forward,
        landed,
    )
    mixed_ref[...] = acc_ref[...].astype(jnp.bfloat16)

    small_cols = out_small_ref.shape[0]

    def chunk_product(chunk):
        rows = pl.ds(pl.multiple_of(chunk * part, OFFSET_ROWS), part)
        return jnp.dot(
            mixed_ref[rows, :small_cols], out_small_ref[...], preferred_element_type=jnp.float32
        ) + jnp.dot(
            mixed_ref[rows, small_cols:], out_large_ref[...], preferred_element_type=jnp.float32
        )

    def to(place, block, source, target, send_sem, arrive_sem):
        return pltpu.make_async_remote_copy(
            src_ref=source,
            dst_ref=target,
            send_sem=send_sem,
            recv_sem=arrive_sem,
            device_id=(place, block),
            device_id_type=MESH,
        )

    core_copies = tuple(
        to(sp, partner, core_out_ref.at[i], core_in_ref.at[i], core_sem.at[0, i], core_sem.at[1, i])
        for i in range(2)
    )
    side_copy = to(sp, across, side_out_ref, side_in_ref, side_sem.at[0], side_sem.at[1])
    core_out_ref[0] = chunk_product((1 - y) * 2 + 1 - core).astype(jnp.bfloat16)
    core_copies[0].start()
    stream_ref[...] = chunk_product(across)
    core_copies[0].wait_recv()
    side_out_ref[...] = (stream_ref[...] + core_in_ref[0].astype(jnp.float32)).astype(jnp.bfloat16)
    side_copy.start()
    core_out_ref[1] = chunk_product(y * 2 + 1 - core).astype(jnp.bfloat16)
    core_copies[1].start()
    stream_ref[...] = chunk_product(tp)
    core_copies[1].wait_recv()
    stream_ref[...] += core_in_ref[1].astype(jnp.float32)
    side_copy.wait_recv()
    attended = (stream_ref[...] + side_in_ref[...].astype(jnp.float32)).astype(jnp.bfloat16)
    stream = residual_ref[...].astype(jnp.float32) + attended.astype(jnp.float32)
    stream_ref[...] = stream
    scale = lax.rsqrt(jnp.mean(stream * stream, axis=-1, keepdims=True) + 1e-06)
    my_rows = pl.ds(pl.multiple_of(core * part, OFFSET_ROWS), part)
    other_rows = pl.ds(pl.multiple_of((1 - core) * part, OFFSET_ROWS), part)
    my_chip = low * 2 + y
    normed_ref[my_chip, my_rows, :] = (
        stream_ref[...] * scale * gain_ref[...].astype(jnp.float32)
    ).astype(jnp.bfloat16)

    def chip_of(step):
        dz, dy = 1 - step // 2, 1 - step % 2
        low_there = (low + dz) % 2
        y_there = (y + dy) % 2
        place = (z - low + low_there) * width + x
        return low_there * 2 + y_there, place, y_there * 2 + core

    def spread(step):
        _, place, block = chip_of(step)
        here = normed_ref.at[my_chip, my_rows, :]
        return to(place, block, here, here, gather_sem.at[step], gather_in_sem.at[my_chip, 0])

    def to_partner(chip, step):
        here = normed_ref.at[chip, my_rows, :]
        return to(sp, partner, here, here, pass_sem.at[step], gather_in_sem.at[chip, 1])

    def from_partner(chip):
        here = normed_ref.at[chip, other_rows, :]
        return to(sp, partner, here, here, pass_sem.at[0], gather_in_sem.at[chip, 1])

    for step in (2, 1, 0):
        spread(step).start()
    to_partner(my_chip, 3).start()

    def far_up(index, nothing):
        column_weights(height - 1 - index, start)
        return nothing

    def from_below(index, nothing):
        pass_on(z - 1 - index)
        return nothing

    lax.fori_loop(0, height - 2 - z, far_up, 0)
    lax.fori_loop(0, z, from_below, 0)
    for step in (2, 1, 0):
        chip, _, _ = chip_of(step)
        here = normed_ref.at[chip, my_rows, :]
        to(sp, partner, here, here, gather_sem.at[step], gather_in_sem.at[chip, 0]).wait_recv()
        to_partner(chip, step).start()

    for copy in own_weights:
        copy.wait()

    def row_arrived(row, nothing):
        for copy in weight_copies(row * width + 1 - x, low, sp, row_w_sem.at[row], True):
            wait_recv(copy)
        return nothing

    lax.fori_loop(0, height, row_arrived, 0)
    place_of = lax.broadcasted_iota(jnp.int32, (2 * part, share), 1)
    counted = place_of >= low * (share - spare)

    def swap_copy(step):
        return to(
            sp, partner, swap_out_ref.at[step], swap_in_ref.at[step], swap_sem.at[0, step], swap_sem.at[1, step]
        )

    def sum_copy(step):
        _, place, block = chip_of(step)
        return to(place, block, sum_ref.at[step], sum_in_ref.at[step], sum_sem.at[0, step], sum_sem.at[1, step])

    def add_partner(step):
        swap_copy(step).wait_recv()
        total = sum_ref[step].astype(jnp.float32) + swap_in_ref[step].astype(jnp.float32)
        sum_ref[step] = total.astype(jnp.bfloat16)

    def feed(step, nothing):
        chip, _, _ = chip_of(step)
        from_partner(chip).wait_recv()
        rows = normed_ref[chip]
        gate = jnp.dot(rows, wg_ref[...], preferred_element_type=jnp.float32)
        upper = jnp.dot(rows, wu_ref[...], preferred_element_type=jnp.float32)
        hidden = jnp.where(counted, jax.nn.silu(gate) * upper, 0.0).astype(jnp.bfloat16)
        down = jnp.dot(hidden, wd_ref[...], preferred_element_type=jnp.float32)
        first = down[:part].astype(jnp.bfloat16)
        second = down[part:].astype(jnp.bfloat16)

        @pl.when(core == 0)
        def _():
            sum_ref[step] = first
            swap_out_ref[step] = second

        @pl.when(core == 1)
        def _():
            sum_ref[step] = second
            swap_out_ref[step] = first

        swap_copy(step).start()

        @pl.when(step > 0)
        def _():
            add_partner(step - 1)
            sum_copy(step - 1).start()

        return nothing

    lax.fori_loop(0, 4, feed, 0)
    add_partner(3)
    total = sum_ref[3].astype(jnp.float32)
    for step in range(3):
        sum_copy(step).wait_recv()
        total += sum_in_ref[step].astype(jnp.float32)
    mixer = total.astype(jnp.bfloat16).astype(jnp.float32)
    out_ref[...] = (stream_ref[...] + mixer).astype(jnp.bfloat16)

    travel.finish()

    @pl.when((x == 1) & (z == height - 2))
    def _():
        shift_copy().wait_send()

    for copy in core_copies:
        wait_send(copy)
    wait_send(side_copy)
    for step in range(3):
        wait_send(spread(step))
        wait_send(sum_copy(step))
    for step in range(4):
        wait_send(to_partner(my_chip, step))
        wait_send(swap_copy(step))

    def weights_sent(row, nothing):
        @pl.when(row != z)
        def _():
            column_weights(row, wait_send)

        row_weights(row, wait_send, True)
        return nothing

    lax.fori_loop(0, height, weights_sent, 0)


def fused_layer(
    n_sp,
    width,
    query_small,
    query_large,
    packed,
    n_small,
    n_large,
    out_small,
    out_large,
    residual,
    norm_gain,
    gate_weight,
    up_weight,
    down_weight,
):
    tokens = query_small.shape[0]
    cols = query_small.shape[1] + query_large.shape[1]
    heads = n_small + n_large
    height = n_sp // width
    part, model = residual.shape
    hidden = gate_weight.shape[1]
    share = -(-hidden // (2 * LANES)) * LANES
    vmem = pl.BlockSpec(memory_space=pltpu.VMEM)
    hbm = pl.BlockSpec(memory_space=pl.ANY)
    piece = (part, model)
    bf16 = jnp.bfloat16
    dma = pltpu.SemaphoreType.DMA
    return pl.pallas_call(
        functools.partial(layer_kernel, n_sp, width, n_small, n_large),
        out_shape=jax.ShapeDtypeStruct(piece, bf16),
        in_specs=[vmem, vmem, hbm, vmem, vmem, vmem, vmem, hbm, hbm, hbm],
        out_specs=vmem,
        scratch_shapes=[
            pltpu.VMEM((TILE, TILE), bf16),
            pltpu.VMEM((heads, tokens, LANES), bf16),
            pltpu.VMEM((tokens, cols), jnp.float32),
            pltpu.VMEM((heads, tokens, 1), jnp.float32),
            pltpu.VMEM((n_sp,) + packed.shape, bf16),
            pltpu.VMEM((model, share), bf16),
            pltpu.VMEM((model, share), bf16),
            pltpu.VMEM((share, model), bf16),
            pltpu.VMEM((tokens, cols), bf16),
            pltpu.VMEM((2,) + piece, bf16),
            pltpu.VMEM((2,) + piece, bf16),
            pltpu.VMEM(piece, bf16),
            pltpu.VMEM(piece, bf16),
            pltpu.VMEM((4, 2 * part, model), bf16),
            pltpu.VMEM(piece, jnp.float32),
            pltpu.VMEM((4,) + piece, bf16),
            pltpu.VMEM((4,) + piece, bf16),
            pltpu.VMEM((4,) + piece, bf16),
            pltpu.VMEM((3,) + piece, bf16),
            dma,
            dma((height,)),
            dma((height, width)),
            dma((n_sp,)),
            dma,
            dma((3,)),
            dma((height, 3)),
            dma((height, 3)),
            dma((n_sp, 3)),
            dma((2, 2)),
            dma((2,)),
            dma((3,)),
            dma((4,)),
            dma((4, 2)),
            dma((2, 4)),
            dma((2, 3)),
        ],
        compiler_params=pltpu.CompilerParams(
            vmem_limit_bytes=67043328, collective_id=1, has_side_effects=True
        ),
        name="fused_layer",
    )(
        query_small,
        query_large,
        packed,
        out_small,
        out_large,
        residual,
        norm_gain.reshape(1, model),
        gate_weight,
        up_weight,
        down_weight,
    )


def on_device(n_sp, width, *args):
    return layer(n_sp, width, *args)


def layer(
    n_sp,
    width,
    query_small,
    key_small,
    value_small,
    offset_small,
    query_large,
    key_large,
    value_large,
    offset_large,
    out_small,
    out_large,
    residual,
    norm_gain,
    gate_weight,
    up_weight,
    down_weight,
):
    if fits(n_sp, width, value_small.shape[0], gate_weight.shape[1]):
        return fused_layer(
            n_sp,
            width,
            query_small,
            query_large,
            pack(
                (key_small, value_small, key_large, value_large),
                jnp.concatenate([offset_small, offset_large], axis=0),
            ),
            offset_small.shape[0],
            offset_large.shape[0],
            out_small,
            out_large,
            residual,
            norm_gain,
            gate_weight,
            up_weight,
            down_weight,
        )
    packed = pack(
        (key_small, value_small, key_large, value_large),
        jnp.concatenate([offset_small, offset_large], axis=0),
    )
    gate_full = lax.all_gather(gate_weight, "sp", axis=0, tiled=True)
    up_full = lax.all_gather(up_weight, "sp", axis=0, tiled=True)
    down_full = lax.all_gather(down_weight, "sp", axis=1, tiled=True)
    out_rows = jnp.concatenate([out_small, out_large], axis=0)
    mixed = attend(
        n_sp, width, query_small, query_large, packed, offset_small.shape[0], offset_large.shape[0]
    )
    attended = lax.psum_scatter(
        jnp.dot(mixed, out_rows, preferred_element_type=jnp.float32).astype(jnp.bfloat16),
        "tp",
        scatter_dimension=0,
        tiled=True,
    ).astype(jnp.float32)
    stream = residual.astype(jnp.float32) + rounded(attended)
    normed = rms_norm(stream, norm_gain)
    normed_rows = lax.all_gather(normed, "tp", axis=0, tiled=True)
    gate = jnp.dot(normed_rows, gate_full, preferred_element_type=jnp.float32)
    upper = jnp.dot(normed_rows, up_full, preferred_element_type=jnp.float32)
    hidden = (jax.nn.silu(gate) * upper).astype(jnp.bfloat16)
    summed = lax.psum_scatter(
        jnp.dot(hidden, down_full, preferred_element_type=jnp.float32).astype(jnp.bfloat16),
        "tp",
        scatter_dimension=0,
        tiled=True,
    ).astype(jnp.float32)
    return (stream + rounded(summed)).astype(jnp.bfloat16)


def solution(mesh):
    return jax.shard_map(
        functools.partial(on_device, mesh.shape["sp"], column_count(mesh)),
        mesh=mesh,
        in_specs=(
            P("sp", "tp"),
            P("sp", "tp"),
            P("sp", "tp"),
            P("tp", "sp"),
            P("sp", "tp"),
            P("sp", "tp"),
            P("sp", "tp"),
            P("tp", "sp"),
            P("tp", None),
            P("tp", None),
            P(("sp", "tp"), None),
            P(),
            P("sp", "tp"),
            P("sp", "tp"),
            P("tp", "sp"),
        ),
        out_specs=P(("sp", "tp"), None),
        check_vma=False,
    )
```
